256 devices in a mesh: sp: 64 (over z, y, core), tp: 4 (over x).
Axes of the slice: x: 4, y: 4, z: 8, core: 2. Of those that a mesh axis runs over, the one named last changes fastest.
Arguments:
- resid: bfloat16 [24576, 2048], P(('sp', 'tp')), may hold values from -6 to 6
- pool_in: bfloat16 [24576, 1024], P('sp', 'tp'), may hold values from -6 to 6
- pool_mix: bfloat16 [4, 256, 256], P('tp'), may hold values from -0.375 to 0.375
- pool_scale: float32 [1024], P('tp'), may hold values from 0.1 to 1.9
- w_pool_out: bfloat16 [1024, 2048], P('tp'), may hold values from -0.1875 to 0.1875
- norm_gains: float32 [3, 2048], replicated, may hold values from 0.1 to 1.9
- route_experts: int32 [24576, 2], P('sp'), may hold values from 0 to 63, all different within a row; in each aligned block of 96 rows (0 to 95, 96 to 191, ...) at most 3 rows name the same one
- route_weights: float32 [24576, 2], P('sp'), may hold values from 0.2 to 1
- w_gate: bfloat16 [64, 2048, 3584], P('sp', None, 'tp'), may hold values from -0.125 to 0.125
- w_up: bfloat16 [64, 2048, 3584], P('sp', None, 'tp'), may hold values from -0.125 to 0.125
- w_down: bfloat16 [64, 3584, 2048], P('sp', 'tp'), may hold values from -0.09375 to 0.09375
Outputs:
- layer_out: bfloat16 [24576, 2048], P(('sp', 'tp'))
The draws below stay inside these ranges and needn't reach their ends.
Inputs may be any that keep to these rules, and one draw needn't show every extreme that they name: `route_experts`: in each aligned block of 96 rows (the rows of one device after the mixer) every expert is named exactly 3 times; the 2 experts of a row differ.
All inputs are finite; a program needn't handle non-finite values.
Results may differ from the reference program's by a relative error of at most 0.017.
Values may be sent and summed in bfloat16 or wider, within the bound.
No kernel may reach another device: no remote copies, remote signals or barrier semaphores. Data moves between devices by JAX's collectives and lax.ppermute only.
A program may use at most 64 MiB of HBM per device.

```python
import math
import jax
import jax.numpy as jnp
import numpy as np
from jax import lax

D = 2048
POOL_GROUPS = 4
GROUP_DIM = 256
FF_E = 3584
TOP = 2
POOL_WIDTH = 1024
EXPERTS = 64
ROWS = 96
CAP = 3
TOKENS = 24576
N_TP = 4


def block_scale(rng, shape, cuts, smallest, largest):
    level, own = 1.0, jax.random.fold_in(rng, 6)
    for axis_at, blocks in cuts:
        draws = jnp.exp(jax.random.uniform(jax.random.fold_in(own, axis_at), (blocks,), jnp.float32, smallest / len(cuts), largest / len(cuts)))
        level = level * jnp.repeat(draws, shape[axis_at] // blocks).reshape([-1 if axis == axis_at else 1 for axis in range(len(shape))])
    return level


def assign_block(key, own, number, rows, number_of, top, bound, skew):
    sequence = jax.random.permutation(key, number_of)
    crowded, ordinary = shares(number_of, rows * top, bound, skew, True), shares(number_of, rows * top, bound, skew, False)
    places = jnp.arange(number_of)

    def named(tallies, rotation):
        used = int((tallies > 0).sum())
        fixed = max(1, used // 4)
        moved = fixed + (places - fixed + rotation * (used - fixed)) % max(1, number_of - fixed)
        return jnp.zeros((number_of,), jnp.int32).at[sequence[jnp.where(places < fixed, places, moved)]].set(jnp.asarray(tallies, jnp.int32))

    tallies = jnp.where(number % 4 == 0, named(crowded, number // 4), named(ordinary, number - number // 4 - 1))
    mixed = jax.random.permutation(jax.random.fold_in(own, 3), number_of)
    source_of, receiver = mixed[0:number_of // 2 * 2:2], mixed[1:number_of // 2 * 2:2]
    room = jnp.minimum(tallies[source_of] - 1, bound - tallies[receiver]) // 2
    room = jnp.where((source_of == sequence[0]) | (receiver == sequence[0]) | (tallies[receiver] == 0), 0, jnp.maximum(room, 0))
    moved = jax.random.randint(jax.random.fold_in(own, 4), (number_of // 2,), 0, 1 << 20) % (room + 1)
    tallies = tallies.at[source_of].add(-moved).at[receiver].add(moved)
    labels = jnp.searchsorted(jnp.cumsum(tallies), jnp.arange(rows * top), side="right").astype(jnp.int32)
    listing = labels.reshape(top, rows).T
    listing = listing[jax.random.permutation(jax.random.fold_in(own, 1), rows)]
    rotation = jax.random.randint(jax.random.fold_in(own, 2), (rows, 1), 0, top)
    return jnp.take_along_axis(listing, (jnp.arange(top)[None, :] + rotation) % top, axis=1)


def shares(number_of, total, limit, skew, full):
    weights = [(1 << 20) // math.isqrt(grade ** skew) + 1 for grade in range(1, number_of + 1)]
    largest = limit if full else min(limit, max(-(-total // number_of), total * weights[0] // sum(weights)))
    least = 1 if total - largest >= number_of - 1 else 0
    holding, spare = [largest] + [least] * (number_of - 1), total - largest - least * (number_of - 1)
    while spare > 0:
        movable = [i for i in range(1, number_of) if holding[i] < largest] or [i for i in range(1, number_of) if holding[i] < limit]
        pool, budget = sum([weights[i] for i in movable]), spare
        for i in movable:
            more = min(limit - holding[i], max(1, budget * weights[i] // pool), spare)
            holding[i] = holding[i] + more
            spare = spare - more
    return np.array(holding)


def noise(stream_key, extent, scale, most, cuts=(), kind=jnp.bfloat16):
    level = block_scale(stream_key, extent, cuts, -0.22, 0.18) if cuts else 1.0
    result = jax.random.normal(stream_key, extent, jnp.float32) * scale * level
    return jnp.minimum(jnp.maximum(result, -most), most).astype(kind)


def setup_inputs(seed: int = 0) -> dict:
    splits = jax.random.split(jax.random.key(seed), 12)
    resid = noise(splits[0], (TOKENS, D), 1.0, 6.0, ((0, 256),))
    pool_in = noise(splits[1], (TOKENS, POOL_WIDTH), 1.0, 6.0, ((0, 64), (1, 4)))
    pool_mix = noise(splits[2], (POOL_GROUPS, GROUP_DIM, GROUP_DIM), GROUP_DIM ** -0.5, 0.375, ((0, 4),))
    pool_scale = jnp.clip(1.0 + 0.18 * jax.random.normal(splits[3], (POOL_WIDTH,), jnp.float32), 0.1, 1.9)
    w_pool_out = noise(splits[4], (POOL_WIDTH, D), POOL_WIDTH ** -0.5, 0.1875, ((0, 4),))
    norm_gains = jnp.clip(1.0 + 0.18 * jax.random.normal(splits[5], (3, D), jnp.float32), 0.1, 1.9)
    route_experts_keys = jax.random.split(jax.random.fold_in(splits[6], 1), TOKENS // ROWS)
    route_experts_turns = jax.random.permutation(jax.random.fold_in(splits[6], 3), TOKENS // ROWS)
    route_experts = jax.vmap(lambda own, number: assign_block(jax.random.fold_in(splits[6], 2), own, number, ROWS, EXPERTS, TOP, CAP, 2))(route_experts_keys, route_experts_turns).reshape((TOKENS, TOP))
    route_weights = jnp.clip(0.2 + 0.8 * jax.random.uniform(splits[7], (TOKENS, TOP), jnp.float32) ** block_scale(splits[7], (TOKENS, TOP), ((0, 64),), -0.2, 0.2), 0.2, 1.0)
    w_gate = noise(splits[8], (EXPERTS, D, FF_E), D ** -0.5, 0.125, ((0, 64), (2, 4)))
    w_up = noise(splits[9], (EXPERTS, D, FF_E), D ** -0.5, 0.125, ((0, 64), (2, 4)))
    w_down = noise(splits[10], (EXPERTS, FF_E, D), FF_E ** -0.5, 0.09375, ((0, 64), (1, 4)))
    return dict(resid=resid, pool_in=pool_in, pool_mix=pool_mix, pool_scale=pool_scale, w_pool_out=w_pool_out, norm_gains=norm_gains, route_experts=route_experts, route_weights=route_weights, w_gate=w_gate, w_up=w_up, w_down=w_down)


EPS = 1e-06

def rms_scale(values, gain):
    return values * lax.rsqrt(lax.optimization_barrier(jnp.mean(values * values, axis=-1, keepdims=True)) + EPS) * gain

def reference(resid, pool_in, pool_mix, pool_scale, w_pool_out, norm_gains, route_experts, route_weights, w_gate, w_up, w_down):
    tokens = pool_in.shape[0]
    position = jnp.arange(tokens, dtype=jnp.int32)
    source = pool_in.astype(jnp.float32).reshape(tokens, POOL_GROUPS, GROUP_DIM)
    running = jnp.cumsum(source, axis=0)
    group_out = []
    for group_index in range(POOL_GROUPS):
        window = 2 ** (group_index + 1)
        window_sum = running[:, group_index]
        lagged = jnp.pad(window_sum, ((window, 0), (0, 0)))[:tokens]
        window_count = jnp.minimum(position + 1, window).astype(jnp.float32)[:, None]
        pooled = ((window_sum - lagged) / window_count - source[:, group_index]).astype(jnp.bfloat16)
        group_out.append(jnp.dot(pooled, pool_mix[group_index], preferred_element_type=jnp.float32))
    mixed_rows = (jnp.concatenate(group_out, axis=1) * pool_scale).astype(jnp.bfloat16)
    width_dev = POOL_WIDTH // N_TP
    mix_sum = jnp.zeros((tokens, D), jnp.float32)
    for slice_index in range(N_TP):
        partial_value = jnp.dot(mixed_rows[:, slice_index * width_dev:(slice_index + 1) * width_dev], w_pool_out[slice_index * width_dev:(slice_index + 1) * width_dev], preferred_element_type=jnp.float32)
        mix_sum = mix_sum + lax.optimization_barrier(partial_value.astype(jnp.bfloat16)).astype(jnp.float32)
    stream = (resid.astype(jnp.float32) + rms_scale(mix_sum, norm_gains[0])).astype(jnp.bfloat16)
    stream_wide = lax.optimization_barrier(stream).astype(jnp.float32)
    normed = rms_scale(stream_wide, norm_gains[1]).astype(jnp.bfloat16)
    picked_ids = route_experts.reshape(-1)
    pick_weight = route_weights.reshape(-1)
    most_rows = tokens // ROWS * CAP
    hidden_dev = FF_E // N_TP

    def one_expert(carried, expert):
        chosen = jnp.argsort((picked_ids != expert).astype(jnp.int32), stable=True)[:most_rows].astype(jnp.int32)
        is_live = picked_ids[chosen] == expert
        token_row = chosen // TOP
        rows_in = normed[token_row]
        gate_out = jnp.dot(rows_in, w_gate[expert], preferred_element_type=jnp.float32)
        up_out = jnp.dot(rows_in, w_up[expert], preferred_element_type=jnp.float32)
        hidden = (jax.nn.silu(gate_out) * up_out).astype(jnp.bfloat16)
        expert_sum = jnp.zeros((most_rows, D), jnp.float32)
        for slice_index in range(N_TP):
            partial_value = jnp.dot(hidden[:, slice_index * hidden_dev:(slice_index + 1) * hidden_dev], w_down[expert][slice_index * hidden_dev:(slice_index + 1) * hidden_dev], preferred_element_type=jnp.float32)
            expert_sum = expert_sum + lax.optimization_barrier(partial_value.astype(jnp.bfloat16)).astype(jnp.float32)
        expert_out = lax.optimization_barrier(expert_sum.astype(jnp.bfloat16)).astype(jnp.float32)
        weight = jnp.where(is_live, pick_weight[chosen], 0.0)
        return (carried.at[token_row].add(weight[:, None] * expert_out), None)
    combined_sum, unused = lax.scan(one_expert, jnp.zeros((tokens, D), jnp.float32), jnp.arange(EXPERTS, dtype=jnp.int32))
    combined = lax.optimization_barrier(combined_sum.astype(jnp.bfloat16)).astype(jnp.float32)
    return (stream_wide + rms_scale(combined, norm_gains[2])).astype(jnp.bfloat16)
```

```python
import jax
import jax.numpy as jnp
from jax import lax
from jax.experimental import pallas as pl
from jax.experimental.pallas import tpu as pltpu
from jax.sharding import Mesh
from jax.sharding import PartitionSpec as P

POOL_GROUPS = 4
TOP = 2
LANES = 128
SP = ("sp_0", "sp_1", "sp_2")
SP_TP = ("sp_0", "sp_1", "sp_2", "tp")
EPS = 1e-06
F32 = jnp.float32
BF16 = jnp.bfloat16


DZ_GROUPS = ((0, 1, 7, 2), (6, 3, 5, 4))


def shift(shard, axis, by):
    peers = lax.axis_size(axis)
    by %= peers
    if by == 0:
        return shard
    return lax.ppermute(shard, axis, [(i, (i + by) % peers) for i in range(peers)])


def from_behind(shard, axis, by):
    peers = lax.axis_size(axis)
    return lax.ppermute(shard, axis, [(i, i + by) for i in range(peers) if 0 <= i + by < peers])


def added(a, b):
    return (a.astype(F32) + b.astype(F32)).astype(BF16)


def ring_scatter_sum(opp, right, left):
    half = opp.shape[0] // 2
    from_left = shift(opp[:half], "tp", 1)
    from_right = shift(opp[half:], "tp", -1)
    left_hi = shift(right[half:], "tp", 1)
    right_lo = shift(left[:half], "tp", -1)
    left_lo = shift(added(right[:half], from_left), "tp", 1)
    right_hi = shift(added(left[half:], from_right), "tp", -1)
    return (left_lo, left_hi, right_lo, right_hi)


def ring_gather(rows):
    half = rows.shape[0] // 2
    lo, hi = rows[:half], rows[half:]
    left_lo = shift(lo, "tp", 1)
    right_hi = shift(hi, "tp", -1)
    left_hi = shift(hi, "tp", 1)
    right_lo = shift(lo, "tp", -1)
    opp_lo = shift(left_lo, "tp", 1)
    opp_hi = shift(right_hi, "tp", -1)
    return (lo, hi, left_lo, left_hi, right_lo, right_hi, opp_lo, opp_hi)


def route_slots(ids):
    picks = ids.shape[0] * TOP
    flat = ids.reshape(-1)
    order = jnp.arange(picks, dtype=jnp.int32)
    earlier = (flat[:, None] == flat[None, :]) & (order[None, :] < order[:, None])
    rank = jnp.sum(earlier.astype(jnp.int32), axis=1)
    ny, nc = lax.axis_size("sp_1"), lax.axis_size("sp_2")
    nz = lax.axis_size("sp_0")
    dz = (flat // (ny * nc) - lax.axis_index("sp_0")) % nz
    dy = (flat // nc - lax.axis_index("sp_1")) % ny
    dc = (flat - lax.axis_index("sp_2")) % nc
    capacity = picks // (nz * ny * nc)
    slot = ((dz * ny + dy) * nc + dc) * capacity + rank
    slot = jnp.minimum(slot, picks - 1)
    holds = slot[None, :] == order[:, None]
    token = jnp.sum(jnp.where(holds, order[None, :] // TOP, 0), axis=1)
    return slot, token


def norm_dispatch_kernel(token_ref, own_ref, llo, lhi, rlo, rhi, resid_ref, gain_ref, stream_ref, out_ref, table_ref):
    rows, width = own_ref.shape
    half = rows // 2
    for k, (left, right) in enumerate(((llo, rlo), (lhi, rhi))):
        part = pl.ds(k * half, half)
        mix = own_ref[part, :].astype(F32) + left[...].astype(F32) + right[...].astype(F32)
        scale = lax.rsqrt(jnp.mean(mix * mix, axis=-1, keepdims=True) + EPS)
        stream = (resid_ref[part, :].astype(F32) + mix * scale * gain_ref[0:1, :]).astype(BF16)
        stream_ref[part, :] = stream
        wide = stream.astype(F32)
        scale = lax.rsqrt(jnp.mean(wide * wide, axis=-1, keepdims=True) + EPS)
        normed = wide * scale * gain_ref[1:2, :]
        table_ref[part] = normed.reshape(half, width // LANES, LANES).astype(BF16)

    def place(s, carry):
        out_ref[s] = table_ref[token_ref[s]]
        return carry

    lax.fori_loop(0, out_ref.shape[0], place, 0, unroll=8)


def norm_dispatch(token, own, pieces, resid, gains):
    rows, width = own.shape
    vmem = pl.BlockSpec(memory_space=pltpu.VMEM)
    return pl.pallas_call(
        norm_dispatch_kernel,
        out_shape=(
            jax.ShapeDtypeStruct((rows, width), BF16),
            jax.ShapeDtypeStruct((rows * TOP, width // LANES, LANES), BF16),
        ),
        in_specs=[pl.BlockSpec(memory_space=pltpu.SMEM)] + [vmem] * 7,
        out_specs=(vmem, vmem),
        scratch_shapes=[pltpu.VMEM((rows, width // LANES, LANES), BF16)],
        name="norm_dispatch",
    )(token, own, *pieces, resid, gains)


def combine_kernel(slot_ref, weight_ref, back_ref, stream_ref, gain_ref, out_ref, sum_ref):
    rows, width = stream_ref.shape

    def one(t, carry):
        first = weight_ref[2 * t] * back_ref[slot_ref[2 * t]].astype(F32)
        second = weight_ref[2 * t + 1] * back_ref[slot_ref[2 * t + 1]].astype(F32)
        sum_ref[t] = (first + second).astype(BF16)
        return carry

    lax.fori_loop(0, rows, one, 0, unroll=4)
    combined = sum_ref[...].astype(F32).reshape(rows, width)
    scale = lax.rsqrt(jnp.mean(combined * combined, axis=-1, keepdims=True) + EPS)
    out_ref[...] = (stream_ref[...].astype(F32) + combined * scale * gain_ref[2:3, :]).astype(BF16)


def combine(slot, weights, back, stream, gains):
    rows, width = stream.shape
    smem, vmem = pl.BlockSpec(memory_space=pltpu.SMEM), pl.BlockSpec(memory_space=pltpu.VMEM)
    return pl.pallas_call(
        combine_kernel,
        out_shape=jax.ShapeDtypeStruct((rows, width), BF16),
        in_specs=[smem, smem, vmem, vmem, vmem],
        out_specs=vmem,
        scratch_shapes=[pltpu.VMEM((rows, width // LANES, LANES), BF16)],
        name="combine",
    )(slot, weights, back, stream, gains)


def to_experts(outgoing, group):
    near = jnp.stack([shift(outgoing[dz], "sp_0", dz) for dz in group])
    ny = near.shape[1]
    near = jnp.stack([shift(near[:, dy], "sp_1", dy) for dy in range(ny)])
    near = jnp.stack([shift(near[:, :, dc], "sp_2", dc) for dc in range(near.shape[2])])
    return near


def from_experts(results, group):
    near = jnp.stack([shift(results[dc], "sp_2", -dc) for dc in range(results.shape[0])], axis=2)
    near = jnp.stack([shift(near[dy], "sp_1", -dy) for dy in range(near.shape[0])], axis=1)
    return [shift(near[k], "sp_0", -dz) for k, dz in enumerate(group)]


def expert_rows(rows_in, w_gate, w_up, w_down):
    gate_out = jnp.dot(rows_in, w_gate, preferred_element_type=F32)
    up_out = jnp.dot(rows_in, w_up, preferred_element_type=F32)
    hidden = (jax.nn.silu(gate_out) * up_out).astype(BF16)
    return jnp.dot(hidden, w_down, preferred_element_type=F32).astype(BF16)


def on_device(
    resid, pool_in, pool_mix, pool_scale, w_pool_out, norm_gains, route_experts, route_weights, w_gate, w_up, w_down
):
    tok_dev = pool_in.shape[0]
    width = w_pool_out.shape[1]
    n_tp = lax.axis_size("tp")
    tp = lax.axis_index("tp")
    own_count = tok_dev // n_tp
    reach_rows = 2**POOL_GROUPS - 1
    prior_rows = from_behind(pool_in[tok_dev - reach_rows :], SP, 1)
    extended = jnp.concatenate([prior_rows, pool_in], axis=0)
    out_index = lax.broadcasted_iota(jnp.int32, (tok_dev, tok_dev + reach_rows), 0)
    in_index = lax.broadcasted_iota(jnp.int32, (tok_dev, tok_dev + reach_rows), 1)
    distance = out_index + reach_rows - in_index
    position = lax.axis_index(SP) * tok_dev + lax.broadcasted_iota(jnp.int32, (tok_dev, 1), 0)
    window = jnp.left_shift(jnp.int32(2), tp)
    band_mask = ((distance >= 0) & (distance < window)).astype(BF16)
    window_sum = jnp.dot(band_mask, extended, preferred_element_type=F32)
    window_count = jnp.minimum(position + 1, window).astype(F32)
    pooled = (window_sum / window_count - pool_in.astype(F32)).astype(BF16)
    group_out = jnp.dot(pooled, pool_mix[0], preferred_element_type=F32)
    mixed_rows = (group_out * pool_scale).astype(BF16)

    def bound_for(offset):
        rows = lax.dynamic_slice_in_dim(mixed_rows, ((tp + offset) % n_tp) * own_count, own_count, 0)
        return jnp.dot(rows, w_pool_out, preferred_element_type=F32).astype(BF16)

    opp = bound_for(2)
    pieces = ring_scatter_sum(opp, bound_for(1), bound_for(3))
    own_start = tp * own_count
    own_routes = lax.dynamic_slice_in_dim(route_experts, own_start, own_count, 0)
    own_weights = lax.dynamic_slice_in_dim(route_weights, own_start, own_count, 0)
    slot, token = route_slots(own_routes)
    stream, outgoing = norm_dispatch(token, bound_for(0), pieces, resid, norm_gains)

    nz, ny, nc = (lax.axis_size(a) for a in SP)
    outgoing = outgoing.reshape(nz, ny, nc, -1, width // LANES, LANES)
    back = [None] * nz
    for group in DZ_GROUPS:
        arrived = to_experts(outgoing, group)
        rows = ring_gather(arrived.reshape(-1, width))
        partial = expert_rows(jnp.concatenate(rows, axis=0), w_gate[0], w_up[0], w_down[0])
        own, left, right, opp = (partial[k * len(partial) // 4 : (k + 1) * len(partial) // 4] for k in range(4))
        left_lo, left_hi, right_lo, right_hi = ring_scatter_sum(opp, right, left)
        from_left = jnp.concatenate([left_lo, left_hi], axis=0).astype(F32)
        from_right = jnp.concatenate([right_lo, right_hi], axis=0).astype(F32)
        summed = (own.astype(F32) + from_left + from_right).astype(BF16)
        for dz, block in zip(group, from_experts(summed.reshape(arrived.shape), group)):
            back[dz] = block
    back = jnp.stack(back).reshape(-1, width // LANES, LANES)
    return combine(slot, own_weights.reshape(-1), back, stream, norm_gains)


def solution(mesh):
    finer = Mesh(mesh.devices.reshape(8, 4, 2, mesh.shape["tp"]), ("sp_0", "sp_1", "sp_2", "tp"))
    placed = (
        P(SP_TP, None),
        P(SP, "tp"),
        P("tp", None, None),
        P("tp"),
        P("tp", None),
        P(),
        P(SP, None),
        P(SP, None),
        P(SP, None, "tp"),
        P(SP, None, "tp"),
        P(SP, "tp", None),
    )
    return jax.shard_map(
        on_device, mesh=finer, in_specs=placed, out_specs=P(SP_TP, None), check_vma=False
    )
```

```python
import jax
import jax.numpy as jnp
from jax import lax
from jax.experimental import pallas as pl
from jax.experimental.pallas import tpu as pltpu
from jax.sharding import Mesh
from jax.sharding import PartitionSpec as P


POOL_GROUPS = 4
TOP = 2
LANES = 128
SP = ("sp_0", "sp_1", "sp_2")
SP_TP = ("sp_0", "sp_1", "sp_2", "tp")
EPS = 1e-06
F32 = jnp.float32
BF16 = jnp.bfloat16


CHUNKS = (1, 2)


def shift(shard, axis, by):
    peers = lax.axis_size(axis)
    return lax.ppermute(shard, axis, [(i, (i + by) % peers) for i in range(peers)])


def from_behind(shard, axis, by):
    peers = lax.axis_size(axis)
    return lax.ppermute(shard, axis, [(i, i + by) for i in range(peers) if 0 <= i + by < peers])


def added(a, b):
    return (a.astype(F32) + b.astype(F32)).astype(BF16)


def ring_scatter_sum(opp, right, left):
    half = opp.shape[0] // 2
    from_left = shift(opp[:half], "tp", 1)
    from_right = shift(opp[half:], "tp", -1)
    to_right = jnp.concatenate([added(right[:half], from_left), right[half:]], axis=0)
    to_left = jnp.concatenate([left[:half], added(left[half:], from_right)], axis=0)
    return shift(to_right, "tp", 1), shift(to_left, "tp", -1)


def ring_gather(rows):
    half = rows.shape[0] // 2
    left = shift(rows, "tp", 1)
    right = shift(rows, "tp", -1)
    left_lo, right_hi = left[:half], right[half:]
    opp_lo = shift(left_lo, "tp", 1)
    opp_hi = shift(right_hi, "tp", -1)
    return rows, left, right, opp_lo, opp_hi


def route_slots(ids):
    picks = ids.shape[0] * TOP
    flat = ids.reshape(-1)
    order = jnp.arange(picks, dtype=jnp.int32)
    earlier = (flat[:, None] == flat[None, :]) & (order[None, :] < order[:, None])
    rank = jnp.sum(earlier.astype(jnp.int32), axis=1)
    capacity = sum(CHUNKS)
    experts = picks // capacity
    slot, first = flat * 0, 0
    for rows in CHUNKS:
        slot = jnp.where(rank >= first, first * experts + flat * rows + rank - first, slot)
        first += rows
    holds = (flat * capacity + rank)[None, :] == order[:, None]
    token = jnp.sum(jnp.where(holds, order[None, :] // TOP, 0), axis=1)
    return jnp.minimum(slot, picks - 1), jnp.minimum(token, ids.shape[0] - 1)


def norm_dispatch_kernel(token_ref, own_ref, left_ref, right_ref, resid_ref, gain_ref, stream_ref, out_ref, table_ref):
    rows, width = own_ref.shape
    half = rows // 2
    for k in range(2):
        part = pl.ds(k * half, half)
        mix = own_ref[part, :].astype(F32) + left_ref[part, :].astype(F32) + right_ref[part, :].astype(F32)
        scale = lax.rsqrt(jnp.mean(mix * mix, axis=-1, keepdims=True) + EPS)
        stream = (resid_ref[part, :].astype(F32) + mix * scale * gain_ref[0:1, :]).astype(BF16)
        stream_ref[part, :] = stream
        wide = stream.astype(F32)
        scale = lax.rsqrt(jnp.mean(wide * wide, axis=-1, keepdims=True) + EPS)
        normed = wide * scale * gain_ref[1:2, :]
        table_ref[part] = normed.reshape(half, width // LANES, LANES).astype(BF16)

    def place(s, carry):
        out_ref[s] = table_ref[token_ref[s]]
        return carry

    lax.fori_loop(0, out_ref.shape[0], place, 0, unroll=8)


def norm_dispatch(token, own, left, right, resid, gains):
    rows, width = own.shape
    tiles = width // LANES
    vmem = pl.BlockSpec(memory_space=pltpu.VMEM)
    return pl.pallas_call(
        norm_dispatch_kernel,
        out_shape=(
            jax.ShapeDtypeStruct((rows, width), BF16),
            jax.ShapeDtypeStruct((rows * TOP, tiles, LANES), BF16),
        ),
        in_specs=[pl.BlockSpec(memory_space=pltpu.SMEM)] + [vmem] * 5,
        out_specs=(vmem, vmem),
        scratch_shapes=[pltpu.VMEM((rows, tiles, LANES), BF16)],
        name="norm_dispatch",
    )(token, own, left, right, resid, gains)


def combine_kernel(slot_ref, weight_ref, stream_ref, gain_ref, *rest):
    *back_refs, out_ref, back_ref, sum_ref, sems = rest
    rows, width = stream_ref.shape
    copies, first = [], 0
    for k, part_ref in enumerate(back_refs):
        to = back_ref.at[pl.ds(first, part_ref.shape[0])]
        copies.append(pltpu.make_async_copy(part_ref, to, sems.at[k]))
        copies[-1].start()
        first += part_ref.shape[0]
    for copy in copies:
        copy.wait()

    def one(t, carry):
        first = weight_ref[2 * t] * back_ref[slot_ref[2 * t]].astype(F32)
        second = weight_ref[2 * t + 1] * back_ref[slot_ref[2 * t + 1]].astype(F32)
        sum_ref[t] = (first + second).astype(BF16)
        return carry

    lax.fori_loop(0, rows, one, 0, unroll=4)
    combined = sum_ref[...].astype(F32).reshape(rows, width)
    scale = lax.rsqrt(jnp.mean(combined * combined, axis=-1, keepdims=True) + EPS)
    out_ref[...] = (stream_ref[...].astype(F32) + combined * scale * gain_ref[2:3, :]).astype(BF16)


def combine(slot, weights, backs, stream, gains):
    rows, width = stream.shape
    tiles = width // LANES
    smem, vmem = pl.BlockSpec(memory_space=pltpu.SMEM), pl.BlockSpec(memory_space=pltpu.VMEM)
    return pl.pallas_call(
        combine_kernel,
        out_shape=jax.ShapeDtypeStruct((rows, width), BF16),
        in_specs=[smem, smem, vmem, vmem] + [pl.BlockSpec(memory_space=pl.ANY)] * len(backs),
        out_specs=vmem,
        scratch_shapes=[
            pltpu.VMEM((rows * TOP, tiles, LANES), BF16),
            pltpu.VMEM((rows, tiles, LANES), BF16),
            pltpu.SemaphoreType.DMA((len(backs),)),
        ],
        name="combine",
    )(slot, weights, stream, gains, *backs)


def exchanged(blocks):
    return lax.all_to_all(blocks, SP, 0, 0, tiled=True)


def expert_rows(rows_in, w_gate, w_up, w_down):
    gate_out = jnp.dot(rows_in, w_gate, preferred_element_type=F32)
    up_out = jnp.dot(rows_in, w_up, preferred_element_type=F32)
    hidden = (jax.nn.silu(gate_out) * up_out).astype(BF16)
    return jnp.dot(hidden, w_down, preferred_element_type=F32).astype(BF16)


def layer(
    resid, pool_in, pool_mix, pool_scale, w_pool_out, norm_gains, route_experts, route_weights, w_gate, w_up, w_down
):
    tok_dev = pool_in.shape[0]
    width = w_pool_out.shape[1]
    n_tp = lax.axis_size("tp")
    tp = lax.axis_index("tp")
    own_count = tok_dev // n_tp
    reach_rows = 2**POOL_GROUPS - 1
    prior_rows = from_behind(pool_in[tok_dev - reach_rows :], SP, 1)
    extended = jnp.concatenate([prior_rows, pool_in], axis=0)
    out_index = lax.broadcasted_iota(jnp.int32, (tok_dev, tok_dev + reach_rows), 0)
    in_index = lax.broadcasted_iota(jnp.int32, (tok_dev, tok_dev + reach_rows), 1)
    distance = out_index + reach_rows - in_index
    position = lax.axis_index(SP) * tok_dev + lax.broadcasted_iota(jnp.int32, (tok_dev, 1), 0)
    window = jnp.left_shift(jnp.int32(2), tp)
    band_mask = ((distance >= 0) & (distance < window)).astype(BF16)
    window_sum = jnp.dot(band_mask, extended, preferred_element_type=F32)
    window_count = jnp.minimum(position + 1, window).astype(F32)
    pooled = (window_sum / window_count - pool_in.astype(F32)).astype(BF16)
    group_out = jnp.dot(pooled, pool_mix[0], preferred_element_type=F32)
    mixed_rows = (group_out * pool_scale).astype(BF16)

    def bound_for(offset):
        rows = lax.dynamic_slice_in_dim(mixed_rows, ((tp + offset) % n_tp) * own_count, own_count, 0)
        return jnp.dot(rows, w_pool_out, preferred_element_type=F32).astype(BF16)

    opp = bound_for(2)
    from_left, from_right = ring_scatter_sum(opp, bound_for(1), bound_for(3))
    own_start = tp * own_count
    own_routes = lax.dynamic_slice_in_dim(route_experts, own_start, own_count, 0)
    own_weights = lax.dynamic_slice_in_dim(route_weights, own_start, own_count, 0)
    slot, token = route_slots(own_routes)
    stream, outgoing = norm_dispatch(token, bound_for(0), from_left, from_right, resid, norm_gains)

    experts = lax.axis_size(SP)
    arrived = exchanged(outgoing.reshape(experts, -1, LANES))
    arrived = arrived.reshape(experts, sum(CHUNKS), -1, LANES)
    backs, first = [], 0
    for k, rank_count in enumerate(CHUNKS):
        chunk = arrived[:, first : first + rank_count]
        rows = chunk.reshape(-1, width)
        first += rank_count
        gathered = ring_gather(rows)
        count = len(rows)
        if k == 0:
            done = expert_rows(jnp.concatenate(gathered, axis=0), w_gate[0], w_up[0], w_down[0])
            own, left, right, opp = (done[j * count : (j + 1) * count] for j in range(4))
        else:
            done = expert_rows(jnp.concatenate(gathered[:3], axis=0), w_gate[0], w_up[0], w_down[0])
            own, left, right = (done[j * count : (j + 1) * count] for j in range(3))
            opp = expert_rows(jnp.concatenate(gathered[3:], axis=0), w_gate[0], w_up[0], w_down[0])
        from_left, from_right = ring_scatter_sum(opp, right, left)
        summed = (own.astype(F32) + from_left.astype(F32) + from_right.astype(F32)).astype(BF16)
        summed = summed.reshape(experts, -1, LANES)
        backs.append(exchanged(summed).reshape(-1, width // LANES, LANES))
    return combine(slot, own_weights.reshape(-1), backs, stream, norm_gains)


def solution(mesh):
    finer = Mesh(mesh.devices.reshape(8, 4, 2, mesh.shape["tp"]), ("sp_0", "sp_1", "sp_2", "tp"))
    placed = (
        P(SP_TP, None),
        P(SP, "tp"),
        P("tp", None, None),
        P("tp"),
        P("tp", None),
        P(),
        P(SP, None),
        P(SP, None),
        P(SP, None, "tp"),
        P(SP, None, "tp"),
        P(SP, "tp", None),
    )
    return jax.shard_map(layer, mesh=finer, in_specs=placed, out_specs=P(SP_TP, None), check_vma=False)
```
